32 devices in a mesh: sp: 8 (over z, y), tp: 4 (over x, core).
Axes of the slice: x: 2, y: 2, z: 4, core: 2. Of those that a mesh axis runs over, the one named last changes fastest.
Arguments:
- queries: bfloat16 [4096, 2048], P('sp', 'tp'), may hold values from -6 to 6
- keys: bfloat16 [4096, 2048], P('sp', 'tp'), may hold values from -6 to 6
- values: bfloat16 [4096, 2048], P('sp', 'tp'), may hold values from -6 to 6
- output_gate_logits: bfloat16 [4096, 2048], P('sp', 'tp'), may hold values from -6 to 6
- decay_gate_logits: float32 [2, 4096, 16], P(None, 'sp', 'tp'), may hold values from -6 to 6
- write_strength_logits: float32 [2, 4096, 16], P(None, 'sp', 'tp'), may hold values from -7 to -4
- extra_log_decay: float32 [2, 4096, 16], P(None, 'sp', 'tp'), may hold values from -2.1 to 0
- head_decay_rate: float32 [2, 16], P(None, 'tp'), may hold values from 0 to 0.04
- head_norm_gain: bfloat16 [128], replicated, may hold values from 0.099609375 to 1.8984375
- output_weight: bfloat16 [2048, 4096], P('tp'), may hold values from -0.125 to 0.125
- residual: bfloat16 [4096, 4096], P(('sp', 'tp')), may hold values from -6 to 6
- expert_norm_gain: bfloat16 [4096], replicated, may hold values from 0.099609375 to 1.8984375
- selected_experts: int32 [4096, 2], P(('sp', 'tp')), may hold values from 0 to 7, all different within a row; in each aligned block of 128 rows (0 to 127, 128 to 255, ...) at most 48 rows name the same one
- router_chosen_scores: float32 [4096, 2], P(('sp', 'tp')), may hold values from -6 to 6
- gate_up_weight: bfloat16 [8, 4096, 1536], P('sp', None, 'tp'), may hold values from -0.75 to 0.75
- linear_up_weight: bfloat16 [8, 4096, 1536], P('sp', None, 'tp'), may hold values from -0.375 to 0.375
- down_weight: bfloat16 [8, 1536, 4096], P('sp', 'tp'), may hold values from -0.009765625 to 0.009765625
Outputs:
- block_out: bfloat16 [4096, 4096], P(('sp', 'tp'))
The draws below stay inside these ranges and needn't reach their ends.
Inputs may be any that keep to these rules, and one draw needn't show every extreme that they name: `selected_experts`: each row names 2 different experts. In each aligned block of rows that one device holds, no expert is named by more than 48 rows, and in every draw some expert is named by exactly 48 rows of some block.
All inputs are finite; a program needn't handle non-finite values.
Results may differ from the reference program's by a relative error of at most 0.02.
Values may be sent and summed in bfloat16 or wider, within the bound.
A program may use at most 128 MiB of HBM per device.

```python
import math
import jax
import jax.numpy as jnp
import numpy as np
from jax import lax

D = 4096
HEADS = 16
HEAD_DIM = 128
WIDTH = 2048
FF = 1536
TOPK = 2
EXPERTS = 8
BLOCK = 128
TOK_DEV = 512
SEQ = 4096
CAP = 48
N_SP = 8
N_TP = 4


def draw_head_decay_rate(key, part):
    chooser = jax.random.uniform(jax.random.fold_in(key, 11), (2, HEADS), jnp.float32)
    slow_rate = jnp.exp(jax.random.uniform(jax.random.fold_in(key, 12), (2, HEADS), jnp.float32, math.log(0.1), math.log(0.5))) / SEQ
    fast_rate = jnp.exp(jax.random.uniform(jax.random.fold_in(key, 13), (2, HEADS), jnp.float32, math.log(1.0 / 90.0), math.log(1.0 / 27.0)))
    slow_share = 0.5
    return jnp.where(chooser < slow_share, slow_rate, fast_rate).astype(jnp.float32)


def draw_decay_gate_logits(key, part):
    nblocks = SEQ // TOK_DEV
    offset = jax.random.uniform(jax.random.fold_in(key, 21), (2, nblocks, HEADS), jnp.float32, -1.0, 1.5)
    offset_full = jnp.repeat(offset, TOK_DEV, axis=1)
    noise = jnp.clip(jax.random.normal(jax.random.fold_in(key, 23), (2, SEQ, HEADS), jnp.float32), -4.0, 4.0)
    return (offset_full + noise).astype(jnp.float32)


def draw_extra_log_decay(key, part):
    spots = jax.random.randint(jax.random.fold_in(key, 31), (2, 3, HEADS), 0, SEQ)
    depth = jnp.log(jax.random.uniform(jax.random.fold_in(key, 32), (2, 3, HEADS), jnp.float32, 0.5, 0.8))
    position = jnp.arange(SEQ)[None, :, None, None]
    hits = position == spots[:, None, :, :]
    return jnp.sum(jnp.where(hits, depth[:, None, :, :], 0.0), axis=2).astype(jnp.float32)


def level_of(stream_key, dims, split, least, largest):
    level = 1.0
    for axis_at, shards_of in split:
        heights = jax.random.uniform(jax.random.fold_in(jax.random.fold_in(stream_key, 6), axis_at), (shards_of,), jnp.float32, least / len(split), largest / len(split))
        level = level * jnp.repeat(jnp.exp(heights), dims[axis_at] // shards_of).reshape((-1,) + (1,) * (len(dims) - 1 - axis_at))
    return level


def assign_block(key, own, number, rows, amount, top, limit, skew):
    order = jax.random.permutation(key, amount)
    crowded, usual = load_shares(amount, rows * top, limit, skew, True), load_shares(amount, rows * top, limit, skew, False)
    places = jnp.arange(amount)

    def named(lengths, offset_by):
        used = int((lengths > 0).sum())
        fixed = max(1, used // 4)
        moved = fixed + (places - fixed + offset_by * (used - fixed)) % max(1, amount - fixed)
        return jnp.zeros((amount,), jnp.int32).at[order[jnp.where(places < fixed, places, moved)]].set(jnp.asarray(lengths, jnp.int32))

    lengths = jnp.where(number % 4 == 0, named(crowded, number // 4), named(usual, number - number // 4 - 1))
    mixed = jax.random.permutation(jax.random.fold_in(own, 3), amount)
    giver, taker = mixed[0:amount // 2 * 2:2], mixed[1:amount // 2 * 2:2]
    slack = jnp.minimum(lengths[giver] - 1, limit - lengths[taker]) // 2
    slack = jnp.where((giver == order[0]) | (taker == order[0]) | (lengths[taker] == 0), 0, jnp.maximum(slack, 0))
    moved = jax.random.randint(jax.random.fold_in(own, 4), (amount // 2,), 0, 1 << 20) % (slack + 1)
    lengths = lengths.at[giver].add(-moved).at[taker].add(moved)
    members = jnp.searchsorted(jnp.cumsum(lengths), jnp.arange(rows * top), side="right").astype(jnp.int32)
    table = members.reshape(top, rows).T
    table = table[jax.random.permutation(jax.random.fold_in(own, 1), rows)]
    offset_by = jax.random.randint(jax.random.fold_in(own, 2), (rows, 1), 0, top)
    return jnp.take_along_axis(table, (jnp.arange(top)[None, :] + offset_by) % top, axis=1)


def load_shares(number_of, total, most, lean, full):
    loads = [(1 << 20) // math.isqrt(grade ** lean) + 1 for grade in range(1, number_of + 1)]
    largest = most if full else min(most, max(-(-total // number_of), total * loads[0] // sum(loads)))
    least = 1 if total - largest >= number_of - 1 else 0
    counts, rest = [largest] + [least] * (number_of - 1), total - largest - least * (number_of - 1)
    while rest > 0:
        candidates = [i for i in range(1, number_of) if counts[i] < largest] or [i for i in range(1, number_of) if counts[i] < most]
        mass, left = sum([loads[i] for i in candidates]), rest
        for i in candidates:
            addition = min(most - counts[i], max(1, left * loads[i] // mass), rest)
            counts[i] = counts[i] + addition
            rest = rest - addition
    return np.array(counts)


def centred(key, shape, scale, reach, cuts=(), kind=jnp.bfloat16):
    entries = scale * jax.random.normal(key, shape, jnp.float32)
    if cuts:
        entries = entries * level_of(key, shape, cuts, -0.22, 0.18)
    return jnp.clip(entries, -reach, reach).astype(kind)


def setup_inputs(seed: int = 0) -> dict:
    key_of = jax.random.split(jax.random.key(seed), 18)
    queries = centred(key_of[0], (SEQ, WIDTH), 1.0, 6.0, ((0, 8), (1, 4)))
    keys = centred(key_of[1], (SEQ, WIDTH), 1.0, 6.0, ((0, 8), (1, 4)))
    values = centred(key_of[2], (SEQ, WIDTH), 1.0, 6.0, ((0, 8), (1, 4)))
    output_gate_logits = centred(key_of[3], (SEQ, WIDTH), 1.0, 6.0, ((0, 8), (1, 4)))
    decay_gate_logits = draw_decay_gate_logits(jax.random.fold_in(key_of[17], 71), 0)
    write_strength_logits = jnp.clip(-7.0 + 3.0 * jax.random.uniform(key_of[5], (2, SEQ, HEADS), jnp.float32) ** level_of(key_of[5], (2, SEQ, HEADS), ((1, 8), (2, 4)), -0.2, 0.2), -7.0, -4.0)
    extra_log_decay = draw_extra_log_decay(jax.random.fold_in(key_of[17], 71), 0)
    head_decay_rate = draw_head_decay_rate(jax.random.fold_in(key_of[17], 71), 0)
    head_norm_gain = jnp.clip(1.0 + 0.18 * jax.random.normal(key_of[8], (HEAD_DIM,), jnp.float32), 0.099609375, 1.8984375).astype(jnp.bfloat16)
    output_weight = centred(key_of[9], (WIDTH, D), WIDTH ** -0.5, 0.125, ((0, 4),))
    residual = centred(key_of[10], (SEQ, D), 1.0, 6.0, ((0, 32),))
    expert_norm_gain = jnp.clip(1.0 + 0.18 * jax.random.normal(key_of[11], (D,), jnp.float32), 0.099609375, 1.8984375).astype(jnp.bfloat16)
    selected_experts_keys = jax.random.split(jax.random.fold_in(key_of[12], 1), SEQ // (TOK_DEV // N_TP))
    selected_experts_turns = jax.random.permutation(jax.random.fold_in(key_of[12], 3), SEQ // (TOK_DEV // N_TP))
    selected_experts = jax.vmap(lambda own, number: assign_block(jax.random.fold_in(key_of[12], 2), own, number, TOK_DEV // N_TP, EXPERTS, TOPK, CAP, 2))(selected_experts_keys, selected_experts_turns).reshape((SEQ, TOPK))
    router_chosen_scores = centred(key_of[13], (SEQ, TOPK), 1.0, 6.0, ((0, 32),), jnp.float32)
    gate_up_weight = centred(key_of[14], (EXPERTS, D, FF), (D // 64) ** -0.5, 0.75, ((0, 8), (2, 4)))
    linear_up_weight = centred(key_of[15], (EXPERTS, D, FF), (D // 16) ** -0.5, 0.375, ((0, 8), (2, 4)))
    down_weight = centred(key_of[16], (EXPERTS, FF, D), (FF * 256) ** -0.5, 0.009765625, ((0, 8), (1, 4)))
    return {"queries": queries, "keys": keys, "values": values, "output_gate_logits": output_gate_logits, "decay_gate_logits": decay_gate_logits, "write_strength_logits": write_strength_logits, "extra_log_decay": extra_log_decay, "head_decay_rate": head_decay_rate, "head_norm_gain": head_norm_gain, "output_weight": output_weight, "residual": residual, "expert_norm_gain": expert_norm_gain, "selected_experts": selected_experts, "router_chosen_scores": router_chosen_scores, "gate_up_weight": gate_up_weight, "linear_up_weight": linear_up_weight, "down_weight": down_weight}


highest = lax.Precision.HIGHEST

def unit_rows(tensor):
    return tensor * lax.rsqrt(lax.optimization_barrier(jnp.sum(tensor * tensor, axis=-1, keepdims=True)) + 1e-06)

def prepare(query_blk, key_blk, value_blk, log_blk, beta_blk):
    cumulative = jnp.cumsum(log_blk, axis=-1)
    position = jnp.arange(log_blk.shape[-1])
    inclusive = position[:, None] >= position[None, :]
    strict = position[:, None] > position[None, :]
    log_gap = cumulative[..., :, None] - cumulative[..., None, :]
    decay_mat = jnp.where(inclusive, jnp.exp(jnp.where(inclusive, log_gap, 0.0)), 0.0)
    key_beta = key_blk * beta_blk[..., None]
    lower_part = jnp.where(strict, jnp.einsum('hnid,hnjd->hnij', key_beta, key_blk, precision=highest) * decay_mat, 0.0)
    lower_mat = lower_part + jnp.eye(log_blk.shape[-1], dtype=jnp.float32)
    corrected = lax.linalg.triangular_solve(lower_mat, value_blk * beta_blk[..., None], left_side=True, lower=True, unit_diagonal=True)
    weighted = lax.linalg.triangular_solve(lower_mat, key_beta * jnp.exp(cumulative)[..., None], left_side=True, lower=True, unit_diagonal=True)
    block_decay = cumulative[..., -1]
    key_end = key_blk * jnp.exp(block_decay[..., None] - cumulative)[..., None]
    query_decay = query_blk * jnp.exp(cumulative)[..., None]
    query_key = jnp.where(inclusive, jnp.einsum('hnid,hnjd->hnij', query_blk, key_blk, precision=highest) * decay_mat, 0.0)
    return (corrected, weighted, key_end, block_decay, query_decay, query_key)

def block_sweep(parts, state, transfer, track_map, emit_out):
    by_block = tuple((jnp.moveaxis(tensor, 1, 0) for tensor in parts))

    def block_step(carried, block_parts):
        state_now, transfer_now = carried
        corrected, weighted, key_end, block_decay, query_decay, query_key = block_parts
        carry_scale = jnp.exp(block_decay)[:, None, None]
        fresh_values = corrected - jnp.einsum('hid,hde->hie', weighted, state_now, precision=highest)
        state_next = carry_scale * state_now + jnp.einsum('hid,hie->hde', key_end, fresh_values, precision=highest)
        emitted = ()
        if emit_out:
            emitted = emitted + (jnp.einsum('hid,hde->hie', query_decay, state_now, precision=highest) + jnp.einsum('hij,hje->hie', query_key, fresh_values, precision=highest),)
        transfer_next = transfer_now
        if track_map:
            moved_map = jnp.einsum('hid,hde->hie', weighted, transfer_now, precision=highest)
            transfer_next = carry_scale * transfer_now - jnp.einsum('hid,hie->hde', key_end, moved_map, precision=highest)
            if emit_out:
                emitted = emitted + (jnp.einsum('hid,hde->hie', query_decay, transfer_now, precision=highest) - jnp.einsum('hij,hje->hie', query_key, moved_map, precision=highest),)
        return ((state_next, transfer_next), emitted)
    return lax.scan(block_step, (state, transfer), by_block)

def one_direction(query_heads, key_heads, value_heads, log_heads, beta_heads):
    head_count = query_heads.shape[0]
    nblocks = query_heads.shape[1] // BLOCK

    def to_blocks(tensor):
        return tensor.reshape((head_count, nblocks, BLOCK) + tensor.shape[2:])
    parts = prepare(to_blocks(query_heads), to_blocks(key_heads), to_blocks(value_heads), to_blocks(log_heads), to_blocks(beta_heads))
    zero_state = jnp.zeros((head_count, HEAD_DIM, HEAD_DIM), jnp.float32)
    finals, emitted = block_sweep(parts, zero_state, zero_state, False, True)
    return jnp.moveaxis(emitted[0], 0, 1).reshape(head_count, -1, HEAD_DIM)

def reference(queries, keys, values, output_gate_logits, decay_gate_logits, write_strength_logits, extra_log_decay, head_decay_rate, head_norm_gain, output_weight, residual, expert_norm_gain, selected_experts, router_chosen_scores, gate_up_weight, linear_up_weight, down_weight):
    seq_len = queries.shape[0]

    def split_heads(tensor):
        return tensor.astype(jnp.float32).reshape(seq_len, HEADS, HEAD_DIM).transpose(1, 0, 2)

    def reverse_tokens(tensor):
        return jnp.flip(tensor, axis=1)
    query_heads = unit_rows(split_heads(queries)) * HEAD_DIM ** (-0.5)
    key_heads = unit_rows(split_heads(keys))
    value_heads = split_heads(values)
    decay_logarithm = (-head_decay_rate[:, None, :] * jax.nn.softplus(decay_gate_logits) + extra_log_decay).transpose(0, 2, 1)
    beta_gate = jax.nn.sigmoid(write_strength_logits).transpose(0, 2, 1)
    forward_out = one_direction(query_heads, key_heads, value_heads, decay_logarithm[0], beta_gate[0])
    backward_out = reverse_tokens(one_direction(reverse_tokens(query_heads), reverse_tokens(key_heads), reverse_tokens(value_heads), reverse_tokens(decay_logarithm[1]), reverse_tokens(beta_gate[1])))
    summed_heads = (forward_out + backward_out).transpose(1, 0, 2)
    scaled_heads = summed_heads * lax.rsqrt(lax.optimization_barrier(jnp.mean(summed_heads * summed_heads, axis=-1, keepdims=True)) + 1e-06) * head_norm_gain.astype(jnp.float32)
    gate_heads = output_gate_logits.astype(jnp.float32).reshape(seq_len, HEADS, HEAD_DIM)
    head_mix = (scaled_heads * jax.nn.silu(gate_heads)).reshape(seq_len, WIDTH).astype(jnp.bfloat16)
    head_piece = WIDTH // N_TP
    mix_sum = jnp.zeros((seq_len, D), jnp.float32)
    for piece_idx in range(N_TP):
        partial_sum = jnp.dot(head_mix[:, piece_idx * head_piece:(piece_idx + 1) * head_piece].astype(jnp.float32), output_weight[piece_idx * head_piece:(piece_idx + 1) * head_piece].astype(jnp.float32), preferred_element_type=jnp.float32).astype(jnp.bfloat16)
        partial_sum = lax.optimization_barrier(partial_sum)
        mix_sum = mix_sum + partial_sum.astype(jnp.float32)
    stream = (residual.astype(jnp.float32) + mix_sum).astype(jnp.bfloat16)
    stream_wide = stream.astype(jnp.float32)
    normed = (stream_wide * lax.rsqrt(lax.optimization_barrier(jnp.mean(stream_wide * stream_wide, axis=-1, keepdims=True)) + 1e-06) * expert_norm_gain.astype(jnp.float32)).astype(jnp.bfloat16)
    route_exp = jnp.exp(router_chosen_scores)
    route_weight = route_exp / lax.optimization_barrier(jnp.sum(route_exp, axis=-1, keepdims=True))
    flat_experts = selected_experts.reshape(-1).astype(jnp.int32)
    flat_weight = route_weight.reshape(-1)
    most_rows = CAP * N_SP * N_TP
    ff_piece = FF // N_TP

    def one_expert(total, expert):
        member = flat_experts == expert
        member_count = jnp.sum(member.astype(jnp.int32))
        where_rows = jnp.nonzero(member, size=most_rows, fill_value=0)[0].astype(jnp.int32)
        live_rows = jnp.arange(most_rows, dtype=jnp.int32) < member_count
        token_rows = (where_rows // TOPK).astype(jnp.int32)
        chosen = normed[token_rows]
        gate_pre = jnp.dot(chosen.astype(jnp.float32), gate_up_weight[expert].astype(jnp.float32), preferred_element_type=jnp.float32)
        linear_pre = jnp.dot(chosen.astype(jnp.float32), linear_up_weight[expert].astype(jnp.float32), preferred_element_type=jnp.float32)
        clipped = jnp.minimum(gate_pre, 7.0)
        hidden_act = (clipped * jax.nn.sigmoid(1.702 * clipped) * (jnp.clip(linear_pre, -7.0, 7.0) + 1.0)).astype(jnp.bfloat16)
        down_rows = down_weight[expert]
        expert_sum = jnp.zeros((most_rows, D), jnp.float32)
        for piece_idx in range(N_TP):
            piece_out = jnp.dot(hidden_act[:, piece_idx * ff_piece:(piece_idx + 1) * ff_piece].astype(jnp.float32), down_rows[piece_idx * ff_piece:(piece_idx + 1) * ff_piece].astype(jnp.float32), preferred_element_type=jnp.float32).astype(jnp.bfloat16)
            piece_out = lax.optimization_barrier(piece_out)
            expert_sum = expert_sum + piece_out.astype(jnp.float32)
        expert_out = lax.optimization_barrier(expert_sum.astype(jnp.bfloat16)).astype(jnp.float32)
        row_weight = jnp.where(live_rows, flat_weight[where_rows], 0.0)
        return (total.at[token_rows].add(expert_out * row_weight[:, None]), None)
    combined, finals = lax.scan(one_expert, jnp.zeros((seq_len, D), jnp.float32), jnp.arange(EXPERTS, dtype=jnp.int32))
    return (stream.astype(jnp.float32) + combined).astype(jnp.bfloat16)
```

```python
import functools

import jax
import jax.numpy as jnp
from jax import lax
from jax.experimental import pallas as pl
from jax.experimental.pallas import tpu as pltpu
from jax.sharding import PartitionSpec as P

HEAD_DIM = 128
TOPK = 2
BLOCK = 128


F32 = jnp.float32
BF16 = jnp.bfloat16
NN = (((1,), (0,)), ((), ()))
NT = (((1,), (1,)), ((), ()))
TN = (((0,), (0,)), ((), ()))


def mm(a, b, dims=NN):
    return lax.dot_general(a.astype(BF16), b.astype(BF16), dims, preferred_element_type=F32)


def local_kernel(
    rate_ref, q_ref, k_ref, v_ref, decay_ref, write_ref, extra_ref, out_ref, map_ref, state_ref
):
    head = pl.program_id(0)
    nblocks = q_ref.shape[0] // BLOCK
    q = q_ref[...].astype(F32)
    k = k_ref[...].astype(F32)
    q = q * (lax.rsqrt(jnp.sum(q * q, axis=-1, keepdims=True) + 1e-06) * HEAD_DIM ** (-0.5))
    k = k * lax.rsqrt(jnp.sum(k * k, axis=-1, keepdims=True) + 1e-06)
    kb = k.astype(BF16)
    qb = q.astype(BF16)
    row = lax.broadcasted_iota(jnp.int32, (BLOCK, BLOCK), 0)
    col = lax.broadcasted_iota(jnp.int32, (BLOCK, BLOCK), 1)
    eye = (row == col).astype(F32)
    lane = lax.broadcasted_iota(jnp.int32, (1, decay_ref.shape[2]), 1)
    picked = lane == head

    def column(ref, d):
        return jnp.sum(jnp.where(picked, ref[d], 0.0), axis=1, keepdims=True)

    units = []
    for d in range(2):
        logits = column(decay_ref, d)
        soft = jnp.maximum(logits, 0.0) + jnp.log1p(jnp.exp(-jnp.abs(logits)))
        log_col = column(extra_ref, d) - rate_ref[d, head] * soft
        beta_col = 1.0 / (1.0 + jnp.exp(-column(write_ref, d)))
        units.append((log_col, beta_col))

    combos = [(n, d) for n in range(nblocks) for d in range(2)]
    scores = {}
    for n in range(nblocks):
        part = slice(n * BLOCK, (n + 1) * BLOCK)
        scores[n] = mm(jnp.concatenate([kb[part], qb[part]], axis=0), kb[part], NT)
    stage = {}
    for n, d in combos:
        part = slice(n * BLOCK, (n + 1) * BLOCK)
        log_col, beta_col = units[d]
        inclusive = row >= col if d == 0 else row <= col
        strict = row > col if d == 0 else row < col
        summed = lax.dot_general(
            inclusive.astype(F32),
            jnp.broadcast_to(log_col[part], (BLOCK, BLOCK)),
            NN,
            precision=lax.Precision.HIGHEST,
            preferred_element_type=F32,
        )
        decay = jnp.exp(jnp.where(inclusive, summed - summed.T, -1e30))
        lower = jnp.where(strict, scores[n][:BLOCK] * decay, 0.0) * beta_col[part]
        attend = (scores[n][BLOCK:] * decay).astype(BF16)
        last = summed[BLOCK - 1 :] if d == 0 else summed[:1]
        grown = jnp.exp(summed)
        stage[n, d] = (lower, attend, grown, jnp.exp(last - summed), jnp.exp(last))
    power = {}
    inverse = {}
    for key in combos:
        lower = stage[key][0]
        power[key] = mm(lower, lower)
        inverse[key] = eye - lower
    size = 2
    while size < BLOCK:
        for key in combos:
            if 2 * size < BLOCK:
                both = mm(jnp.concatenate([inverse[key], power[key]], axis=0), power[key])
                inverse[key] = inverse[key] + both[:BLOCK]
                power[key] = both[BLOCK:]
            else:
                inverse[key] = inverse[key] + mm(inverse[key], power[key])
        size *= 2
    moved = {}
    for n, d in combos:
        part = slice(n * BLOCK, (n + 1) * BLOCK)
        lower, attend, grown, to_end, whole = stage[n, d]
        beta = units[d][1][part]
        values = v_ref[part].astype(F32) * beta
        solved = mm(
            inverse[n, d], jnp.concatenate([values, k[part] * (grown * beta)], axis=1)
        ).astype(BF16)
        seen = mm(attend, solved)
        kept = mm(k[part] * to_end, solved, TN)
        moved[n, d] = (
            seen[:, :HEAD_DIM],
            q[part] * grown - seen[:, HEAD_DIM:],
            kept[:, :HEAD_DIM],
            kept[:, HEAD_DIM:],
            whole,
        )
    outs = [None] * nblocks
    carried = [None, None]
    for step in range(nblocks):
        for d in range(2):
            n = step if d == 0 else nblocks - 1 - step
            part = slice(n * BLOCK, (n + 1) * BLOCK)
            seen, reader, fresh, erase, whole = moved[n, d]
            if step == 0:
                local, through = seen, reader
                new = jnp.concatenate([fresh, whole * eye - erase], axis=1)
            else:
                both = mm(jnp.concatenate([reader, erase], axis=0), carried[d])
                local = seen + both[:BLOCK, :HEAD_DIM]
                through = both[:BLOCK, HEAD_DIM:]
                decayed = jnp.concatenate([whole, whole], axis=1) * carried[d] - both[BLOCK:]
                new = decayed + jnp.concatenate([fresh, jnp.zeros_like(fresh)], axis=1)
            carried[d] = new
            outs[n] = local if outs[n] is None else outs[n] + local
            map_ref[part, d * HEAD_DIM : (d + 1) * HEAD_DIM] = through.astype(BF16)
    for n in range(nblocks):
        out_ref[n * BLOCK : (n + 1) * BLOCK] = outs[n]
    for d in range(2):
        base = 2 * d * HEAD_DIM
        state_ref[base : base + HEAD_DIM] = carried[d][:, HEAD_DIM:].astype(BF16)
        state_ref[base + HEAD_DIM : base + 2 * HEAD_DIM] = carried[d][:, :HEAD_DIM].astype(BF16)


def mix_kernel(here_ref, all_ref, out_ref, map_ref, gate_ref, gain_ref, mix_ref, held_ref):
    count = all_ref.shape[0]
    heads = all_ref.shape[1] // (4 * HEAD_DIM)
    here = here_ref[0]

    held_ref[...] = jnp.zeros_like(held_ref)

    def sweep(d, at):
        new = []
        for h in range(heads):
            base = (4 * h + 2 * d) * HEAD_DIM
            step_map = all_ref[at, base : base + HEAD_DIM, :]
            added = all_ref[at, base + HEAD_DIM : base + 2 * HEAD_DIM, :].astype(F32)
            new.append(mm(step_map, held_ref[h, d]) + added)
        for h in range(heads):
            held_ref[h, d] = new[h]

    @pl.loop(0, here)
    def _(at):
        sweep(0, at)

    @pl.loop(0, count - 1 - here)
    def _(back):
        sweep(1, count - 1 - back)

    for h in range(heads):
        lanes = slice(h * HEAD_DIM, (h + 1) * HEAD_DIM)
        entering = jnp.concatenate([held_ref[h, 0], held_ref[h, 1]], axis=0)
        o = out_ref[:, lanes] + mm(map_ref[:, 2 * h * HEAD_DIM : 2 * (h + 1) * HEAD_DIM], entering)
        scale = lax.rsqrt(jnp.mean(o * o, axis=-1, keepdims=True) + 1e-06)
        gate = gate_ref[:, lanes].astype(F32)
        o = o * scale * gain_ref[...].astype(F32) * (gate / (1.0 + jnp.exp(-gate)))
        mix_ref[:, lanes] = o.astype(BF16)


def exchange(pieces, axis):
    size = lax.axis_size(axis)
    bit = size // 2
    while bit:
        pairs = [(i, i ^ bit) for i in range(size)]
        pieces = pieces + [
            jax.tree.map(lambda leaf: lax.ppermute(leaf, axis, pairs), piece) for piece in pieces
        ]
        bit //= 2
    return pieces


def per_device(
    queries,
    keys,
    values,
    output_gate_logits,
    decay_gate_logits,
    write_strength_logits,
    extra_log_decay,
    head_decay_rate,
    head_norm_gain,
    output_weight,
    residual,
    expert_norm_gain,
    selected_experts,
    router_chosen_scores,
    gate_up_weight,
    linear_up_weight,
    down_weight,
):
    tok_rows, width_dev = queries.shape
    head_count = width_dev // HEAD_DIM

    experts_whole = exchange([(gate_up_weight, linear_up_weight, down_weight)], "tp")
    whole_block = lambda shape: pl.BlockSpec(shape, lambda h: (0,) * len(shape))
    head_block = pl.BlockSpec((tok_rows, HEAD_DIM), lambda h: (0, h))
    local_out, through_maps, state_maps = pl.pallas_call(
        local_kernel,
        grid=(head_count,),
        in_specs=[pl.BlockSpec(memory_space=pltpu.SMEM)]
        + [head_block] * 3
        + [whole_block(decay_gate_logits.shape)] * 3,
        out_specs=[
            head_block,
            pl.BlockSpec((tok_rows, 2 * HEAD_DIM), lambda h: (0, h)),
            pl.BlockSpec((4 * HEAD_DIM, HEAD_DIM), lambda h: (h, 0)),
        ],
        out_shape=[
            jax.ShapeDtypeStruct((tok_rows, width_dev), F32),
            jax.ShapeDtypeStruct((tok_rows, 2 * width_dev), BF16),
            jax.ShapeDtypeStruct((4 * width_dev, HEAD_DIM), BF16),
        ],
        cost_estimate=pl.CostEstimate(
            flops=80 * tok_rows * BLOCK * width_dev, bytes_accessed=100000000, transcendentals=0
        ),
        name="local_kernel",
    )(
        head_decay_rate,
        queries,
        keys,
        values,
        decay_gate_logits,
        write_strength_logits,
        extra_log_decay,
    )
    everything = lax.all_gather(state_maps, "sp")
    head_mix = pl.pallas_call(
        mix_kernel,
        in_specs=[pl.BlockSpec(memory_space=pltpu.SMEM)]
        + [pl.BlockSpec(memory_space=pltpu.VMEM)] * 5,
        out_specs=pl.BlockSpec(memory_space=pltpu.VMEM),
        out_shape=jax.ShapeDtypeStruct((tok_rows, width_dev), BF16),
        scratch_shapes=[pltpu.VMEM((head_count, 2, HEAD_DIM, HEAD_DIM), F32)],
        cost_estimate=pl.CostEstimate(
            flops=8 * tok_rows * BLOCK * width_dev, bytes_accessed=20000000, transcendentals=0
        ),
        name="mix_kernel",
    )(
        lax.axis_index("sp").astype(jnp.int32).reshape(1),
        everything,
        local_out,
        through_maps,
        output_gate_logits,
        head_norm_gain.reshape(1, HEAD_DIM),
    )
    local_rows = residual.shape[0]
    mix_sum = lax.psum_scatter(
        jnp.dot(head_mix, output_weight, preferred_element_type=jnp.float32).astype(jnp.bfloat16),
        "tp",
        scatter_dimension=0,
        tiled=True,
    ).astype(jnp.float32)
    stream = (residual.astype(jnp.float32) + mix_sum).astype(jnp.bfloat16)
    stream_wide = stream.astype(jnp.float32)
    normed = (
        stream_wide
        * lax.rsqrt(jnp.mean(stream_wide * stream_wide, axis=-1, keepdims=True) + 1e-06)
        * expert_norm_gain.astype(jnp.float32)
    ).astype(jnp.bfloat16)
    route_exp = jnp.exp(router_chosen_scores)
    route_weight = route_exp / jnp.sum(route_exp, axis=-1, keepdims=True)
    sp_count = lax.axis_size("sp")
    tp_count = lax.axis_size("tp")
    exp_dev = gate_up_weight.shape[0]
    experts = exp_dev * sp_count
    capacity = 3 * TOPK * tok_rows // (2 * tp_count * experts)
    model_width = normed.shape[1]
    flat_experts = selected_experts.reshape(-1)
    member = (flat_experts[:, None] == jnp.arange(experts, dtype=jnp.int32)[None, :]).astype(
        jnp.int32
    )
    slot_rank = jnp.sum(jnp.cumsum(member, axis=0) * member, axis=1) - 1
    slot_index = flat_experts * capacity + slot_rank
    slot_hot = (
        slot_index[:, None] == jnp.arange(experts * capacity, dtype=jnp.int32)[None, :]
    ).astype(jnp.bfloat16)
    token_hot = jnp.sum(slot_hot.reshape(local_rows, TOPK, experts * capacity), axis=1)
    outgoing = jnp.einsum(
        "rs,rd->sd", token_hot, normed, preferred_element_type=jnp.float32
    ).astype(jnp.bfloat16)
    grouped = outgoing.reshape(sp_count, exp_dev, capacity, model_width)
    arrived = lax.all_to_all(grouped, "sp", split_axis=0, concat_axis=0, tiled=True)
    total = None
    for gate_w, linear_w, down_w in experts_whole:
        gate_pre = jnp.einsum("secd,edf->secf", arrived, gate_w, preferred_element_type=F32)
        linear_pre = jnp.einsum("secd,edf->secf", arrived, linear_w, preferred_element_type=F32)
        clipped = jnp.minimum(gate_pre, 7.0)
        hidden_act = (
            clipped * jax.nn.sigmoid(1.702 * clipped) * (jnp.clip(linear_pre, -7.0, 7.0) + 1.0)
        ).astype(BF16)
        piece = jnp.einsum("secf,efd->secd", hidden_act, down_w, preferred_element_type=F32)
        total = piece if total is None else total + piece
    summed = total.astype(BF16)
    returned = lax.all_to_all(summed, "sp", split_axis=0, concat_axis=0, tiled=True)
    returned = returned.reshape(experts * capacity, model_width)
    picked = jnp.dot(slot_hot, returned, preferred_element_type=jnp.float32).reshape(
        local_rows, TOPK, model_width
    )
    combined = jnp.sum(picked * route_weight[:, :, None], axis=1)
    return (stream_wide + combined).astype(jnp.bfloat16)


def solution(mesh):
    placed = (
        P("sp", "tp"),
        P("sp", "tp"),
        P("sp", "tp"),
        P("sp", "tp"),
        P(None, "sp", "tp"),
        P(None, "sp", "tp"),
        P(None, "sp", "tp"),
        P(None, "tp"),
        P(),
        P("tp", None),
        P(("sp", "tp"), None),
        P(),
        P(("sp", "tp"), None),
        P(("sp", "tp"), None),
        P("sp", None, "tp"),
        P("sp", None, "tp"),
        P("sp", "tp", None),
    )
    return jax.shard_map(
        per_device, mesh=mesh, in_specs=placed, out_specs=P(("sp", "tp"), None), check_vma=False
    )
```

```python
import jax
import jax.numpy as jnp
from jax import lax
from jax.experimental import pallas as pl
from jax.experimental.pallas import tpu as pltpu
from jax.sharding import PartitionSpec as P

HEAD_DIM = 128
TOPK = 2
BLOCK = 128


F32 = jnp.float32
BF16 = jnp.bfloat16
NN = (((1,), (0,)), ((), ()))
NT = (((1,), (1,)), ((), ()))
TN = (((0,), (0,)), ((), ()))


def mm(a, b, dims=NN):
    return lax.dot_general(a.astype(BF16), b.astype(BF16), dims, preferred_element_type=F32)


def local_kernel(
    rate_ref, q_ref, k_ref, v_ref, decay_ref, write_ref, extra_ref, out_ref, map_ref, state_ref
):
    head = pl.program_id(0)
    nblocks = q_ref.shape[0] // BLOCK
    q = q_ref[...].astype(F32)
    k = k_ref[...].astype(F32)
    q = q * (lax.rsqrt(jnp.sum(q * q, axis=-1, keepdims=True) + 1e-06) * HEAD_DIM ** (-0.5))
    k = k * lax.rsqrt(jnp.sum(k * k, axis=-1, keepdims=True) + 1e-06)
    kb = k.astype(BF16)
    qb = q.astype(BF16)
    row = lax.broadcasted_iota(jnp.int32, (BLOCK, BLOCK), 0)
    col = lax.broadcasted_iota(jnp.int32, (BLOCK, BLOCK), 1)
    eye = (row == col).astype(F32)
    lane = lax.broadcasted_iota(jnp.int32, (1, decay_ref.shape[2]), 1)
    picked = lane == head

    def column(ref, d):
        return jnp.sum(jnp.where(picked, ref[d], 0.0), axis=1, keepdims=True)

    units = []
    for d in range(2):
        logits = column(decay_ref, d)
        soft = jnp.maximum(logits, 0.0) + jnp.log1p(jnp.exp(-jnp.abs(logits)))
        log_col = column(extra_ref, d) - rate_ref[d, head] * soft
        beta_col = 1.0 / (1.0 + jnp.exp(-column(write_ref, d)))
        units.append((log_col, beta_col))

    combos = [(n, d) for n in range(nblocks) for d in range(2)]
    scores = {}
    for n in range(nblocks):
        part = slice(n * BLOCK, (n + 1) * BLOCK)
        scores[n] = mm(jnp.concatenate([kb[part], qb[part]], axis=0), kb[part], NT)
    stage = {}
    for n, d in combos:
        part = slice(n * BLOCK, (n + 1) * BLOCK)
        log_col, beta_col = units[d]
        inclusive = row >= col if d == 0 else row <= col
        strict = row > col if d == 0 else row < col
        summed = lax.dot_general(
            inclusive.astype(F32),
            jnp.broadcast_to(log_col[part], (BLOCK, BLOCK)),
            NN,
            precision=lax.Precision.HIGHEST,
            preferred_element_type=F32,
        )
        decay = jnp.exp(jnp.where(inclusive, summed - summed.T, -1e30))
        lower = jnp.where(strict, scores[n][:BLOCK] * decay, 0.0) * beta_col[part]
        attend = (scores[n][BLOCK:] * decay).astype(BF16)
        last = summed[BLOCK - 1 :] if d == 0 else summed[:1]
        grown = jnp.exp(summed)
        stage[n, d] = (lower, attend, grown, jnp.exp(last - summed), jnp.exp(last))
    power = {}
    inverse = {}
    for key in combos:
        lower = stage[key][0]
        power[key] = mm(lower, lower)
        inverse[key] = eye - lower
    size = 2
    while size < BLOCK:
        for key in combos:
            if 2 * size < BLOCK:
                both = mm(jnp.concatenate([inverse[key], power[key]], axis=0), power[key])
                inverse[key] = inverse[key] + both[:BLOCK]
                power[key] = both[BLOCK:]
            else:
                inverse[key] = inverse[key] + mm(inverse[key], power[key])
        size *= 2
    moved = {}
    for n, d in combos:
        part = slice(n * BLOCK, (n + 1) * BLOCK)
        lower, attend, grown, to_end, whole = stage[n, d]
        beta = units[d][1][part]
        values = v_ref[part].astype(F32) * beta
        solved = mm(
            inverse[n, d], jnp.concatenate([values, k[part] * (grown * beta)], axis=1)
        ).astype(BF16)
        seen = mm(attend, solved)
        kept = mm(k[part] * to_end, solved, TN)
        moved[n, d] = (
            seen[:, :HEAD_DIM],
            q[part] * grown - seen[:, HEAD_DIM:],
            kept[:, :HEAD_DIM],
            kept[:, HEAD_DIM:],
            whole,
        )
    outs = [None] * nblocks
    carried = [None, None]
    for step in range(nblocks):
        for d in range(2):
            n = step if d == 0 else nblocks - 1 - step
            part = slice(n * BLOCK, (n + 1) * BLOCK)
            seen, reader, fresh, erase, whole = moved[n, d]
            if step == 0:
                local, through = seen, reader
                new = jnp.concatenate([fresh, whole * eye - erase], axis=1)
            else:
                both = mm(jnp.concatenate([reader, erase], axis=0), carried[d])
                local = seen + both[:BLOCK, :HEAD_DIM]
                through = both[:BLOCK, HEAD_DIM:]
                decayed = jnp.concatenate([whole, whole], axis=1) * carried[d] - both[BLOCK:]
                new = decayed + jnp.concatenate([fresh, jnp.zeros_like(fresh)], axis=1)
            carried[d] = new
            outs[n] = local if outs[n] is None else outs[n] + local
            map_ref[part, d * HEAD_DIM : (d + 1) * HEAD_DIM] = through.astype(BF16)
    for n in range(nblocks):
        out_ref[n * BLOCK : (n + 1) * BLOCK] = outs[n]
    for d in range(2):
        base = 2 * d * HEAD_DIM
        state_ref[base : base + HEAD_DIM] = carried[d][:, HEAD_DIM:].astype(BF16)
        state_ref[base + HEAD_DIM : base + 2 * HEAD_DIM] = carried[d][:, :HEAD_DIM].astype(BF16)


def mix_kernel(here_ref, all_ref, out_ref, map_ref, gate_ref, gain_ref, mix_ref, held_ref):
    count = all_ref.shape[0]
    heads = all_ref.shape[1] // (4 * HEAD_DIM)
    here = here_ref[0]

    held_ref[...] = jnp.zeros_like(held_ref)

    def sweep(d, at):
        new = []
        for h in range(heads):
            base = (4 * h + 2 * d) * HEAD_DIM
            step_map = all_ref[at, base : base + HEAD_DIM, :]
            added = all_ref[at, base + HEAD_DIM : base + 2 * HEAD_DIM, :].astype(F32)
            new.append(mm(step_map, held_ref[h, d]) + added)
        for h in range(heads):
            held_ref[h, d] = new[h]

    @pl.loop(0, here)
    def _(at):
        sweep(0, at)

    @pl.loop(0, count - 1 - here)
    def _(back):
        sweep(1, count - 1 - back)

    for h in range(heads):
        lanes = slice(h * HEAD_DIM, (h + 1) * HEAD_DIM)
        entering = jnp.concatenate([held_ref[h, 0], held_ref[h, 1]], axis=0)
        o = out_ref[:, lanes] + mm(map_ref[:, 2 * h * HEAD_DIM : 2 * (h + 1) * HEAD_DIM], entering)
        scale = lax.rsqrt(jnp.mean(o * o, axis=-1, keepdims=True) + 1e-06)
        gate = gate_ref[:, lanes].astype(F32)
        o = o * scale * gain_ref[...].astype(F32) * (gate / (1.0 + jnp.exp(-gate)))
        mix_ref[:, lanes] = o.astype(BF16)


def exchange(pieces, axis):
    size = lax.axis_size(axis)
    bit = size // 2
    while bit:
        pairs = [(i, i ^ bit) for i in range(size)]
        moved = []
        for piece in pieces:
            leaves = []
            for leaf in piece:
                leaves.append(lax.ppermute(leaf, axis, pairs))
            moved.append(tuple(leaves))
        pieces = pieces + moved
        bit //= 2
    return pieces


def layer(
    queries,
    keys,
    values,
    output_gate_logits,
    decay_gate_logits,
    write_strength_logits,
    extra_log_decay,
    head_decay_rate,
    head_norm_gain,
    output_weight,
    residual,
    expert_norm_gain,
    selected_experts,
    router_chosen_scores,
    gate_up_weight,
    linear_up_weight,
    down_weight,
):
    tok_rows, width_dev = queries.shape
    head_count = width_dev // HEAD_DIM

    experts_whole = exchange([(gate_up_weight, linear_up_weight, down_weight)], "tp")
    whole_block = lambda shape: pl.BlockSpec(shape, lambda h: (0,) * len(shape))
    head_block = pl.BlockSpec((tok_rows, HEAD_DIM), lambda h: (0, h))
    attend = pl.pallas_call(
        local_kernel,
        grid=(head_count,),
        in_specs=[pl.BlockSpec(memory_space=pltpu.SMEM)]
        + [head_block] * 3
        + [whole_block(decay_gate_logits.shape)] * 3,
        out_specs=[
            head_block,
            pl.BlockSpec((tok_rows, 2 * HEAD_DIM), lambda h: (0, h)),
            pl.BlockSpec((4 * HEAD_DIM, HEAD_DIM), lambda h: (h, 0)),
        ],
        out_shape=[
            jax.ShapeDtypeStruct((tok_rows, width_dev), F32),
            jax.ShapeDtypeStruct((tok_rows, 2 * width_dev), BF16),
            jax.ShapeDtypeStruct((4 * width_dev, HEAD_DIM), BF16),
        ],
        cost_estimate=pl.CostEstimate(
            flops=80 * tok_rows * BLOCK * width_dev, bytes_accessed=100000000, transcendentals=0
        ),
        name="local_kernel",
    )
    local_out, through_maps, state_maps = attend(
        head_decay_rate,
        queries,
        keys,
        values,
        decay_gate_logits,
        write_strength_logits,
        extra_log_decay,
    )
    everything = lax.all_gather(state_maps, "sp")
    head_mix = pl.pallas_call(
        mix_kernel,
        in_specs=[pl.BlockSpec(memory_space=pltpu.SMEM)]
        + [pl.BlockSpec(memory_space=pltpu.VMEM)] * 5,
        out_specs=pl.BlockSpec(memory_space=pltpu.VMEM),
        out_shape=jax.ShapeDtypeStruct((tok_rows, width_dev), BF16),
        scratch_shapes=[pltpu.VMEM((head_count, 2, HEAD_DIM, HEAD_DIM), F32)],
        cost_estimate=pl.CostEstimate(
            flops=8 * tok_rows * BLOCK * width_dev, bytes_accessed=20000000, transcendentals=0
        ),
        name="mix_kernel",
    )(
        lax.axis_index("sp").astype(jnp.int32).reshape(1),
        everything,
        local_out,
        through_maps,
        output_gate_logits,
        head_norm_gain.reshape(1, HEAD_DIM),
    )
    local_rows = residual.shape[0]
    mix_sum = lax.psum_scatter(
        jnp.dot(head_mix, output_weight, preferred_element_type=jnp.float32).astype(jnp.bfloat16),
        "tp",
        scatter_dimension=0,
        tiled=True,
    ).astype(jnp.float32)
    stream = (residual.astype(jnp.float32) + mix_sum).astype(jnp.bfloat16)
    stream_wide = stream.astype(jnp.float32)
    normed = (
        stream_wide
        * lax.rsqrt(jnp.mean(stream_wide * stream_wide, axis=-1, keepdims=True) + 1e-06)
        * expert_norm_gain.astype(jnp.float32)
    ).astype(jnp.bfloat16)
    route_exp = jnp.exp(router_chosen_scores)
    route_weight = route_exp / jnp.sum(route_exp, axis=-1, keepdims=True)
    sp_count = lax.axis_size("sp")
    tp_count = lax.axis_size("tp")
    exp_dev = gate_up_weight.shape[0]
    experts = exp_dev * sp_count
    capacity = 3 * TOPK * tok_rows // (2 * tp_count * experts)
    model_width = normed.shape[1]
    flat_experts = selected_experts.reshape(-1)
    member = (flat_experts[:, None] == jnp.arange(experts, dtype=jnp.int32)[None, :]).astype(
        jnp.int32
    )
    slot_rank = jnp.sum(jnp.cumsum(member, axis=0) * member, axis=1) - 1
    slot_index = flat_experts * capacity + slot_rank
    slot_hot = (
        slot_index[:, None] == jnp.arange(experts * capacity, dtype=jnp.int32)[None, :]
    ).astype(jnp.bfloat16)
    token_hot = jnp.sum(slot_hot.reshape(local_rows, TOPK, experts * capacity), axis=1)
    outgoing = jnp.einsum(
        "rs,rd->sd", token_hot, normed, preferred_element_type=jnp.float32
    ).astype(jnp.bfloat16)
    grouped = outgoing.reshape(sp_count, exp_dev, capacity, model_width)
    arrived = lax.all_to_all(grouped, "sp", split_axis=0, concat_axis=0, tiled=True)
    total = None
    for gate_w, linear_w, down_w in experts_whole:
        gate_pre = jnp.einsum("secd,edf->secf", arrived, gate_w, preferred_element_type=F32)
        linear_pre = jnp.einsum("secd,edf->secf", arrived, linear_w, preferred_element_type=F32)
        clipped = jnp.minimum(gate_pre, 7.0)
        hidden_act = (
            clipped * jax.nn.sigmoid(1.702 * clipped) * (jnp.clip(linear_pre, -7.0, 7.0) + 1.0)
        ).astype(BF16)
        piece = jnp.einsum("secf,efd->secd", hidden_act, down_w, preferred_element_type=F32)
        total = piece if total is None else total + piece
    summed = total.astype(BF16)
    returned = lax.all_to_all(summed, "sp", split_axis=0, concat_axis=0, tiled=True)
    returned = returned.reshape(experts * capacity, model_width)
    picked = jnp.dot(slot_hot, returned, preferred_element_type=jnp.float32).reshape(
        local_rows, TOPK, model_width
    )
    combined = jnp.sum(picked * route_weight[:, :, None], axis=1)
    return (stream_wide + combined).astype(jnp.bfloat16)


def solution(mesh):
    placed = (
        P("sp", "tp"),
        P("sp", "tp"),
        P("sp", "tp"),
        P("sp", "tp"),
        P(None, "sp", "tp"),
        P(None, "sp", "tp"),
        P(None, "sp", "tp"),
        P(None, "tp"),
        P(),
        P("tp", None),
        P(("sp", "tp"), None),
        P(),
        P(("sp", "tp"), None),
        P(("sp", "tp"), None),
        P("sp", None, "tp"),
        P("sp", None, "tp"),
        P("sp", "tp", None),
    )
    return jax.shard_map(
        layer,
        mesh=mesh,
        in_specs=placed,
        out_specs=P(("sp", "tp"), None),
        check_vma=False,
    )
```
